32 devices in a mesh: sp: 32 (over z, y, x, core), fs: 1, tp: 1.
Axes of the slice: x: 2, y: 2, z: 4, core: 2. Of those that a mesh axis runs over, the one named last changes fastest.
Arguments:
- tokens: bfloat16 [4096, 2048], P(('fs', 'sp'), 'tp'), may hold values from -450 to 450
- documents: int32 [4096], P(('fs', 'sp')), may hold values from 0 to 3, never falling along the last dimension, each value on 1 to 2048 neighbouring positions
- norm_gain: bfloat16 [2048], P('tp'), may hold values from 0.099609375 to 1.8984375
- out_gate_weight: bfloat16 [2048, 1024], P('sp', 'tp'), may hold values from -0.125 to 0.125
- in_gate_weight: bfloat16 [2048, 1024], P('sp', 'tp'), may hold values from -0.125 to 0.125
- value_weight: bfloat16 [2048, 1024], P('sp', 'tp'), may hold values from -0.125 to 0.125
- conv_taps: bfloat16 [3, 1024], P(None, 'tp'), may hold values from -3.5 to 3.5
- state_in_weight: bfloat16 [2048, 1024], P('sp', 'tp'), may hold values from -0.125 to 0.125
- decay_rate: float32 [64, 64], P('tp'), may hold values from 4e-05 to 2.01
- frequency: float32 [64, 64], P('tp'), may hold values from 0 to 32
- step_log: float32 [64], P('tp'), may hold values from -3.9121 to -1.6094
- input_real: float32 [64, 64, 16], P('tp'), may hold values from -1 to 1
- input_imag: float32 [64, 64, 16], P('tp'), may hold values from -1 to 1
- readout_real: float32 [64, 16, 64], P('tp'), may hold values from -0.75 to 0.75
- readout_imag: float32 [64, 16, 64], P('tp'), may hold values from -0.75 to 0.75
- skip_gain: float32 [1024], P('tp'), may hold values from -4 to 4
- conv_out_weight: bfloat16 [1024, 2048], P('tp', 'sp'), may hold values from -0.125 to 0.125
- state_out_weight: bfloat16 [1024, 2048], P('tp', 'sp'), may hold values from -0.125 to 0.125
Outputs:
- mixed: bfloat16 [4096, 2048], P(('fs', 'sp', 'tp'))
The draws below stay inside these ranges and needn't reach their ends.
All inputs are finite; a program needn't handle non-finite values.
Results may differ from the reference program's by a relative error of at most 0.015.
Values may be sent and summed in bfloat16 or wider, within the bound.
A program may use at most 64 MiB of HBM per device.

```python
import math
import jax
import jax.numpy as jnp
import numpy as np
from jax import lax

D = 2048
CONV = 1024
SSM = 1024
GROUP = 16
STATE = 64
TAPS = 3
BLOCK = 64
TOKENS = 4096
GROUPS = 64
DOCS = 4
DOC_MOST = 2048
N_TP = 1


def draw_tokens(key, part):
    streams = jax.random.split(jax.random.fold_in(key, 11), 4)
    noise = jnp.clip(jax.random.normal(streams[0], (TOKENS, D), jnp.float32), -5.0, 5.0)
    row_scale = jnp.exp(jax.random.uniform(streams[1], (TOKENS, 1), jnp.float32, 0.0, math.log(10.0)))
    col_scale = jnp.exp(jax.random.uniform(streams[2], (1, D), jnp.float32, 0.0, math.log(3.0)))
    upper_half = jnp.arange(D) >= D // 2
    swapped = jax.random.bernoulli(streams[3])
    half_scale = jnp.where(jnp.logical_xor(upper_half, swapped), 3.0, 1.0)
    return (noise * row_scale * col_scale * half_scale[None, :]).astype(jnp.bfloat16)


def rate_table(key):
    streams = jax.random.split(jax.random.fold_in(key, 23), 4)
    step_log = jax.random.uniform(streams[0], (GROUPS,), jnp.float32, math.log(0.02), math.log(0.2))
    share = 0.5
    slow_mask = jax.random.uniform(streams[1], (GROUPS, 1), jnp.float32) < share
    slow_part = jnp.exp(jax.random.uniform(streams[2], (GROUPS, STATE), jnp.float32, math.log(1e-05), math.log(5e-05)))
    fast_part = jnp.exp(jax.random.uniform(streams[3], (GROUPS, STATE), jnp.float32, math.log(0.02), math.log(0.04)))
    product = jnp.where(slow_mask, slow_part, fast_part)
    return (step_log, product / jnp.exp(step_log)[:, None])


def draw_step_log(key, part):
    return rate_table(key)[0]


def draw_decay_rate(key, part):
    return rate_table(key)[1]


def block_levels(key, dims, cuts, low, high):
    loudness, own = 1.0, jax.random.fold_in(key, 6)
    for position, parts in cuts:
        draws = jnp.exp(jax.random.uniform(jax.random.fold_in(own, position), (parts,), jnp.float32, low / len(cuts), high / len(cuts)))
        loudness = loudness * jnp.repeat(draws, dims[position] // parts).reshape([-1 if axis == position else 1 for axis in range(len(dims))])
    return loudness


def split_up(count, total, most, lean):
    loads = [(1 << 20) // math.isqrt(rank ** lean) + 1 for rank in range(2, count + 1)]
    surplus, given = total - most - (count - 1), [1] * (count - 1)
    while surplus > 0:
        candidates = [i for i in range(count - 1) if given[i] < most]
        whole, remaining = sum([loads[i] for i in candidates]), surplus
        for i in candidates:
            more = min(most - given[i], max(1, remaining * loads[i] // whole), surplus)
            given[i] = given[i] + more
            surplus = surplus - more
    return np.array([most] + given)


def uneven(rng, number_of, total, bound, lean):
    if number_of == 2:
        one = jax.random.randint(rng, (), max(1, total - bound), min(bound, total - 1) + 1)
        return jnp.stack([one, total - one])
    tallies = jnp.asarray(split_up(number_of, total, bound, lean), jnp.int32)
    pairs = (number_of - 1) // 2
    giver, receiver = tallies[1:1 + 2 * pairs:2], tallies[2:2 + 2 * pairs:2]
    room = jnp.minimum(giver - 1, bound - receiver)
    passed = jax.random.randint(jax.random.fold_in(rng, 1), (pairs,), 0, 1 << 20) % (room + 1)
    tallies = tallies.at[1:1 + 2 * pairs:2].set(giver - passed).at[2:2 + 2 * pairs:2].set(receiver + passed)
    return tallies[jax.random.permutation(jax.random.fold_in(rng, 2), number_of)]


def bell_draw(stream_key, shape, deviation, reach, cuts=(), held_as=jnp.bfloat16):
    values = deviation * jax.random.normal(stream_key, shape, jnp.float32)
    if cuts:
        values = values * block_levels(stream_key, shape, cuts, -0.22, 0.18)
    return jnp.clip(values, -reach, reach).astype(held_as)


def setup_inputs(seed: int = 0, part: int = 0) -> dict:
    key_list = jax.random.split(jax.random.key(seed), 19)
    part_keys = jax.random.split(jax.random.fold_in(key_list[18], part), 19)
    tokens = draw_tokens(jax.random.fold_in(jax.random.fold_in(key_list[18], part), 71), part)
    documents = jnp.searchsorted(jnp.cumsum(uneven(part_keys[1], DOCS, TOKENS, DOC_MOST, 0)), jnp.arange(TOKENS), side="right").astype(jnp.int32)
    norm_gain = jnp.clip(1.0 + 0.18 * jax.random.normal(key_list[2], (D,), jnp.float32), 0.099609375, 1.8984375).astype(jnp.bfloat16)
    out_gate_weight = bell_draw(key_list[3], (D, CONV), D ** -0.5, 0.125, ((0, 32),))
    in_gate_weight = bell_draw(key_list[4], (D, CONV), D ** -0.5, 0.125, ((0, 32),))
    value_weight = bell_draw(key_list[5], (D, CONV), D ** -0.5, 0.125, ((0, 32),))
    conv_taps = bell_draw(key_list[6], (TAPS, CONV), TAPS ** -0.5, 3.5)
    state_in_weight = bell_draw(key_list[7], (D, SSM), D ** -0.5, 0.125, ((0, 32),))
    decay_rate = draw_decay_rate(jax.random.fold_in(key_list[18], 71), part)
    frequency = jnp.clip(jax.random.uniform(key_list[9], (GROUPS, STATE), jnp.float32, 0.0, 32.0), 0.0, 32.0)
    step_log = draw_step_log(jax.random.fold_in(key_list[18], 71), part)
    input_real = bell_draw(key_list[11], (GROUPS, STATE, GROUP), (2 * GROUP) ** -0.5, 1.0, (), jnp.float32)
    input_imag = bell_draw(key_list[12], (GROUPS, STATE, GROUP), (2 * GROUP) ** -0.5, 1.0, (), jnp.float32)
    readout_real = bell_draw(key_list[13], (GROUPS, GROUP, STATE), STATE ** -0.5, 0.75, (), jnp.float32)
    readout_imag = bell_draw(key_list[14], (GROUPS, GROUP, STATE), STATE ** -0.5, 0.75, (), jnp.float32)
    skip_gain = bell_draw(key_list[15], (SSM,), 1.0, 4.0, (), jnp.float32)
    conv_out_weight = bell_draw(key_list[16], (CONV, D), (CONV + SSM) ** -0.5, 0.125, ((1, 32),))
    state_out_weight = bell_draw(key_list[17], (SSM, D), (CONV + SSM) ** -0.5, 0.125, ((1, 32),))
    return {"tokens": tokens, "documents": documents, "norm_gain": norm_gain, "out_gate_weight": out_gate_weight, "in_gate_weight": in_gate_weight, "value_weight": value_weight, "conv_taps": conv_taps, "state_in_weight": state_in_weight, "decay_rate": decay_rate, "frequency": frequency, "step_log": step_log, "input_real": input_real, "input_imag": input_imag, "readout_real": readout_real, "readout_imag": readout_imag, "skip_gain": skip_gain, "conv_out_weight": conv_out_weight, "state_out_weight": state_out_weight}


EPS = 1e-06

def pair_step(earlier, later):
    dec_real, dec_imag, sum_real, sum_imag = earlier
    late_dec_real, late_dec_imag, late_sum_real, late_sum_imag = later
    return (late_dec_real * dec_real - late_dec_imag * dec_imag, late_dec_real * dec_imag + late_dec_imag * dec_real, late_dec_real * sum_real - late_dec_imag * sum_imag + late_sum_real, late_dec_real * sum_imag + late_dec_imag * sum_real + late_sum_imag)

def ssm_constants(decay_rate, frequency, step_log, input_real, input_imag):
    step_size = jnp.exp(step_log)[:, None]
    damping = decay_rate * step_size
    turning = frequency * step_size
    fading = jnp.exp(-damping)
    coef_real = fading * jnp.cos(turning)
    coef_imag = fading * jnp.sin(turning)
    half_sine = jnp.sin(turning / 2.0)
    less_real = jnp.expm1(-damping) * jnp.cos(turning) - 2.0 * half_sine * half_sine
    denominator = decay_rate * decay_rate + frequency * frequency
    ratio_real = (-less_real * decay_rate + coef_imag * frequency) / denominator
    ratio_imag = (-coef_imag * decay_rate - less_real * frequency) / denominator
    bbar_real = ratio_real[..., None] * input_real - ratio_imag[..., None] * input_imag
    bbar_imag = ratio_real[..., None] * input_imag + ratio_imag[..., None] * input_real
    return (coef_real.reshape(-1), coef_imag.reshape(-1), bbar_real, bbar_imag)

def complex_scan(coef_real, coef_imag, bbar_real, bbar_imag, driven, keep_rows, carry_real, carry_imag, readout_real, readout_imag, block):
    groups, group_size, state_size = readout_real.shape
    row_count = driven.shape[0]
    blocks = row_count // block

    def one_block(carry, pieces):
        start_real, start_imag = carry
        inputs, keeps = pieces
        split_rows = inputs.reshape(block, groups, group_size)
        push_real = jnp.einsum('tgh,gph->tgp', split_rows, bbar_real, precision=lax.Precision.HIGHEST).reshape(block, groups * state_size)
        push_imag = jnp.einsum('tgh,gph->tgp', split_rows, bbar_imag, precision=lax.Precision.HIGHEST).reshape(block, groups * state_size)
        dec_real = coef_real[None, :] * keeps[:, None]
        dec_imag = coef_imag[None, :] * keeps[:, None]
        prod_real, prod_imag, sum_real, sum_imag = lax.associative_scan(pair_step, (dec_real, dec_imag, push_real, push_imag), axis=0)
        held_real = sum_real + prod_real * start_real[None, :] - prod_imag * start_imag[None, :]
        held_imag = sum_imag + prod_real * start_imag[None, :] + prod_imag * start_real[None, :]
        result = jnp.einsum('tgp,ghp->tgh', held_real.reshape(block, groups, state_size), readout_real, precision=lax.Precision.HIGHEST)
        result = result - jnp.einsum('tgp,ghp->tgh', held_imag.reshape(block, groups, state_size), readout_imag, precision=lax.Precision.HIGHEST)
        return ((held_real[-1], held_imag[-1]), result.reshape(block, groups * group_size))
    _, outputs = lax.scan(one_block, (carry_real, carry_imag), (driven.reshape(blocks, block, -1), keep_rows.reshape(blocks, block)))
    return outputs.reshape(row_count, groups * group_size)

def reference(tokens, documents, norm_gain, out_gate_weight, in_gate_weight, value_weight, conv_taps, state_in_weight, decay_rate, frequency, step_log, input_real, input_imag, readout_real, readout_imag, skip_gain, conv_out_weight, state_out_weight):
    values = tokens.astype(jnp.float32)
    scale = lax.rsqrt(lax.optimization_barrier(jnp.mean(values * values, axis=1, keepdims=True)) + EPS)
    normed = (values * scale * norm_gain.astype(jnp.float32)).astype(jnp.bfloat16)
    out_gate = jnp.dot(normed, out_gate_weight, preferred_element_type=jnp.float32).astype(jnp.bfloat16)
    in_gate = jnp.dot(normed, in_gate_weight, preferred_element_type=jnp.float32).astype(jnp.bfloat16)
    value = jnp.dot(normed, value_weight, preferred_element_type=jnp.float32).astype(jnp.bfloat16)
    driven = jnp.dot(normed, state_in_weight, preferred_element_type=jnp.float32).astype(jnp.bfloat16)
    product = (in_gate.astype(jnp.float32) * value.astype(jnp.float32)).astype(jnp.bfloat16)
    margin = TAPS - 1
    padded = jnp.concatenate([jnp.zeros((margin, product.shape[1]), jnp.bfloat16), product], axis=0)
    padded_docs = jnp.concatenate([jnp.full((margin,), -1, jnp.int32), documents], axis=0)
    total = jnp.zeros(product.shape, jnp.float32)
    for index in range(TAPS):
        same_doc = (padded_docs[index:index + TOKENS] == documents).astype(jnp.float32)
        total = total + conv_taps[index].astype(jnp.float32)[None, :] * padded[index:index + TOKENS].astype(jnp.float32) * same_doc[:, None]
    conv_out = (out_gate.astype(jnp.float32) * total).astype(jnp.bfloat16)
    coef_real, coef_imag, bbar_real, bbar_imag = ssm_constants(decay_rate, frequency, step_log, input_real, input_imag)
    keep_rows = jnp.concatenate([jnp.zeros((1,), jnp.float32), (documents[1:] == documents[:-1]).astype(jnp.float32)], axis=0)
    driven_wide = driven.astype(jnp.float32)
    zero_state = jnp.zeros(coef_real.shape, jnp.float32)
    readout = complex_scan(coef_real, coef_imag, bbar_real, bbar_imag, driven_wide, keep_rows, zero_state, zero_state, readout_real, readout_imag, BLOCK)
    ssm_out = jax.nn.gelu(readout + skip_gain[None, :] * driven_wide, approximate=True).astype(jnp.bfloat16)
    conv_width = CONV // N_TP
    ssm_width = SSM // N_TP
    summed = jnp.zeros((TOKENS, D), jnp.float32)
    for index in range(N_TP):
        conv_part = jnp.dot(conv_out[:, index * conv_width:(index + 1) * conv_width], conv_out_weight[index * conv_width:(index + 1) * conv_width], preferred_element_type=jnp.float32)
        ssm_part = jnp.dot(ssm_out[:, index * ssm_width:(index + 1) * ssm_width], state_out_weight[index * ssm_width:(index + 1) * ssm_width], preferred_element_type=jnp.float32)
        summed = summed + (conv_part + ssm_part).astype(jnp.bfloat16).astype(jnp.float32)
    return summed.astype(jnp.bfloat16)
```

```python
import functools
import math

import jax
import jax.numpy as jnp
from jax import lax
from jax.experimental import pallas as pl
from jax.experimental.pallas import tpu as pltpu
from jax.sharding import PartitionSpec as P

D = 2048
TAPS = 3
TILE = 8
REACHES = (1, 2, 4)


EPS = 1e-06


def from_behind(block, axis, distance):
    devices = range(lax.axis_size(axis))
    route = [(i - distance, i) for i in devices if i - distance in devices]
    return lax.ppermute(block, axis, route)


def ssm_constants(decay_rate, frequency, step_log, input_real, input_imag):
    step_size = jnp.exp(step_log)[:, None]
    damping = decay_rate * step_size
    turning = frequency * step_size
    fading = jnp.exp(-damping)
    coef_imag = fading * jnp.sin(turning)
    half_sine = jnp.sin(turning / 2.0)
    less_real = jnp.expm1(-damping) * jnp.cos(turning) - 2.0 * half_sine * half_sine
    denominator = decay_rate * decay_rate + frequency * frequency
    ratio_real = (-less_real * decay_rate + coef_imag * frequency) / denominator
    ratio_imag = (-coef_imag * decay_rate - less_real * frequency) / denominator
    bbar_real = ratio_real[..., None] * input_real - ratio_imag[..., None] * input_imag
    bbar_imag = ratio_real[..., None] * input_imag + ratio_imag[..., None] * input_real
    return (bbar_real, bbar_imag, damping.reshape(-1), turning.reshape(-1))


def spread(rows, group_size):
    lanes, state_size = rows.shape
    reps = lanes // group_size
    wide = jnp.concatenate([rows] * reps, axis=1)
    row = lax.broadcasted_iota(jnp.int32, wide.shape, 0) // group_size
    col = lax.broadcasted_iota(jnp.int32, wide.shape, 1) // state_size
    return jnp.where(row == col, wide, 0.0).astype(jnp.bfloat16)


def scan_rows(u, b_re, b_im, pow_re, pow_im, masks, start_re, start_im, keep):
    push_re = jnp.dot(u, b_re, preferred_element_type=jnp.float32)
    push_im = jnp.dot(u, b_im, preferred_element_type=jnp.float32)
    carry_re, carry_im = start_re, start_im
    for begin in range(0, u.shape[0], TILE):
        x_re = push_re[begin : begin + TILE]
        x_im = push_im[begin : begin + TILE]
        for slot, reach in enumerate(REACHES):
            m = masks[begin : begin + TILE, slot : slot + 1]
            p_re = pow_re[reach - 1 : reach] * m
            p_im = pow_im[reach - 1 : reach] * m
            s_re = pltpu.roll(x_re, reach, 0)
            s_im = pltpu.roll(x_im, reach, 0)
            x_re, x_im = x_re + (p_re * s_re - p_im * s_im), x_im + (p_re * s_im + p_im * s_re)
        m = masks[begin : begin + TILE, len(REACHES) : len(REACHES) + 1]
        p_re, p_im = pow_re * m, pow_im * m
        x_re, x_im = (
            x_re + (p_re * carry_re - p_im * carry_im),
            x_im + (p_re * carry_im + p_im * carry_re),
        )
        carry_re, carry_im = x_re[TILE - 1 :], x_im[TILE - 1 :]
        keep(begin, x_re, x_im)
    return carry_re, carry_im


def ends_body(group_size, u_ref, bre_ref, bim_ref, pre_ref, pim_ref, mask_ref, ere_ref, eim_ref):
    zero = jnp.zeros((1, pre_ref.shape[-1]), jnp.float32)
    end_re, end_im = scan_rows(
        u_ref[...],
        spread(bre_ref[...], group_size),
        spread(bim_ref[...], group_size),
        pre_ref[0],
        pim_ref[0],
        mask_ref[...],
        zero,
        zero,
        lambda begin, x_re, x_im: None,
    )
    ere_ref[0] = end_re
    eim_ref[0] = end_im


def join_body(keep_ref, take_ref, end_ref, dec_ref, sre_ref, sim_ref):
    dec_re, dec_im = dec_ref[0], dec_ref[1]
    s_re = jnp.zeros(dec_re.shape, jnp.float32)
    s_im = s_re
    for turn in range(end_ref.shape[0]):
        keep, take = keep_ref[turn], take_ref[turn]
        n_re = dec_re * s_re - dec_im * s_im + end_ref[turn, 0]
        n_im = dec_re * s_im + dec_im * s_re + end_ref[turn, 1]
        s_re, s_im = keep * s_re + take * n_re, keep * s_im + take * n_im
    sre_ref[...] = s_re
    sim_ref[...] = s_im


def mix_body(
    group_size, u_ref, bre_ref, bim_ref, cre_ref, cim_ref, pre_ref, pim_ref, mask_ref,
    sre_ref, sim_ref, skip_ref, out_ref, hre_ref, him_ref,
):
    def keep(begin, x_re, x_im):
        hre_ref[begin : begin + TILE, :] = x_re
        him_ref[begin : begin + TILE, :] = x_im

    u = u_ref[...]
    scan_rows(
        u,
        spread(bre_ref[...], group_size),
        spread(bim_ref[...], group_size),
        pre_ref[0],
        pim_ref[0],
        mask_ref[...],
        sre_ref[0],
        sim_ref[0],
        keep,
    )
    along = (((1,), (1,)), ((), ()))
    y = lax.dot_general(
        hre_ref[...].astype(jnp.bfloat16),
        spread(cre_ref[...], group_size),
        along,
        preferred_element_type=jnp.float32,
    ) - lax.dot_general(
        him_ref[...].astype(jnp.bfloat16),
        spread(cim_ref[...], group_size),
        along,
        preferred_element_type=jnp.float32,
    )
    y = y + skip_ref[...] * u.astype(jnp.float32)
    out_ref[...] = jax.nn.gelu(y, approximate=True).astype(jnp.bfloat16)


def block_specs(rows, lanes, state_size, span):
    return dict(
        u=pl.BlockSpec((rows, lanes), lambda j: (0, j)),
        mat=pl.BlockSpec((lanes, state_size), lambda j: (j, 0)),
        pow=pl.BlockSpec((1, TILE, span), lambda j: (j, 0, 0)),
        mask=pl.BlockSpec((rows, len(REACHES) + 1), lambda j: (0, 0)),
        state=pl.BlockSpec((1, 1, span), lambda j: (j, 0, 0)),
        skip=pl.BlockSpec((1, lanes), lambda j: (0, j)),
    )


def shards(
    tokens,
    documents,
    norm_gain,
    out_gate_weight,
    in_gate_weight,
    value_weight,
    conv_taps,
    state_in_weight,
    decay_rate,
    frequency,
    step_log,
    input_real,
    input_imag,
    readout_real,
    readout_imag,
    skip_gain,
    conv_out_weight,
    state_out_weight,
):
    row_count = tokens.shape[0]
    groups, state_size = decay_rate.shape
    group_size = input_real.shape[2]
    values = tokens.astype(jnp.float32)
    totals = lax.psum(jnp.sum(values * values, axis=1), "tp")
    scaled = values * lax.rsqrt(totals / D + EPS)[:, None] * norm_gain.astype(jnp.float32)[None, :]
    normed = lax.all_gather(scaled.astype(jnp.bfloat16), "tp", axis=1, tiled=True)
    bbar_real, bbar_imag, damping, turning = ssm_constants(
        decay_rate, frequency, step_log, input_real, input_imag
    )
    doc_float = documents.astype(jnp.float32)
    pieces = (
        lax.all_gather(out_gate_weight, "sp", axis=0, tiled=True),
        lax.all_gather(in_gate_weight, "sp", axis=0, tiled=True),
        lax.all_gather(value_weight, "sp", axis=0, tiled=True),
        lax.all_gather(state_in_weight, "sp", axis=0, tiled=True),
    )
    gate_sum, inner_sum, value_sum, driven_sum = tuple(
        (jnp.dot(normed, piece, preferred_element_type=jnp.float32) for piece in pieces)
    )
    driven = driven_sum.astype(jnp.bfloat16)
    place = lax.axis_index("sp")
    devices = lax.axis_size("sp")
    lasts = lax.all_gather(doc_float[-1], "sp")
    in_last = jnp.where(place > 0, lasts[jnp.maximum(place - 1, 0)], -1.0)
    lanes = math.gcd(groups * group_size, 128)
    blocks = groups * group_size // lanes
    span = lanes // group_size * state_size
    order = jnp.arange(row_count)
    columns = [
        (order % TILE >= reach) & (documents == jnp.roll(documents, reach)) for reach in REACHES
    ]
    before = jnp.concatenate([in_last[None], doc_float[TILE - 1 : -1 : TILE]])
    columns.append(doc_float == jnp.repeat(before, TILE))
    masks = jnp.stack(columns, axis=1).astype(jnp.float32)
    counts = jnp.arange(1, TILE + 1, dtype=jnp.float32)[None, :, None]
    damp = damping.reshape(blocks, 1, span)
    turn = turning.reshape(blocks, 1, span)
    fade = jnp.exp(-counts * damp)
    pow_re, pow_im = fade * jnp.cos(counts * turn), fade * jnp.sin(counts * turn)
    damp, turn = damp[:, 0], turn[:, 0]
    whole = jnp.exp(-row_count * damp)
    decay = jnp.stack([whole * jnp.cos(row_count * turn), whole * jnp.sin(row_count * turn)])
    b_re = jnp.swapaxes(bbar_real, 1, 2).reshape(groups * group_size, state_size)
    b_im = jnp.swapaxes(bbar_imag, 1, 2).reshape(groups * group_size, state_size)
    c_re = readout_real.reshape(groups * group_size, state_size)
    c_im = readout_imag.reshape(groups * group_size, state_size)
    spec = block_specs(row_count, lanes, state_size, span)
    state_shape = jax.ShapeDtypeStruct((blocks, 1, span), jnp.float32)
    ends = pl.pallas_call(
        functools.partial(ends_body, group_size),
        grid=(blocks,),
        in_specs=[spec[k] for k in ("u", "mat", "mat", "pow", "pow", "mask")],
        out_specs=[spec["state"]] * 2,
        out_shape=[state_shape] * 2,
        name="ends",
    )(driven, b_re, b_im, pow_re, pow_im, masks)
    ends = lax.all_gather(jnp.stack([e.reshape(blocks, span) for e in ends]), "sp")
    source = jnp.arange(devices)
    take = ((source < place) & (lasts == in_last)).astype(jnp.float32)
    later = (source >= place).astype(jnp.float32)
    scalar = pl.BlockSpec(memory_space=pltpu.SMEM)
    vector = pl.BlockSpec(memory_space=pltpu.VMEM)
    start_re, start_im = pl.pallas_call(
        join_body,
        in_specs=[scalar, scalar, vector, vector],
        out_specs=[vector] * 2,
        out_shape=[jax.ShapeDtypeStruct((blocks, span), jnp.float32)] * 2,
        name="join",
    )(later, take, ends, decay)
    ssm_out = pl.pallas_call(
        functools.partial(mix_body, group_size),
        grid=(blocks,),
        in_specs=[
            spec[k]
            for k in (
                "u", "mat", "mat", "mat", "mat", "pow", "pow", "mask", "state", "state", "skip",
            )
        ],
        out_specs=spec["u"],
        out_shape=jax.ShapeDtypeStruct(driven.shape, jnp.bfloat16),
        scratch_shapes=[pltpu.VMEM((row_count, span), jnp.float32)] * 2,
        name="mix",
    )(
        driven, b_re, b_im, c_re, c_im, pow_re, pow_im, masks,
        start_re[:, None], start_im[:, None], skip_gain[None],
    )
    out_gate = gate_sum.astype(jnp.bfloat16).astype(jnp.float32)
    in_gate = inner_sum.astype(jnp.bfloat16).astype(jnp.float32)
    value = value_sum.astype(jnp.bfloat16).astype(jnp.float32)
    product = (in_gate * value).astype(jnp.bfloat16)
    margin = TAPS - 1
    tail_same = documents[row_count - margin :] == documents[-1]
    tail_rows = jnp.where(
        tail_same[:, None], product[row_count - margin :], jnp.zeros_like(product[:margin])
    )
    rim_rows = from_behind(tail_rows, "sp", 1)
    padded = jnp.concatenate([rim_rows, product], axis=0)
    padded_docs = jnp.concatenate([jnp.broadcast_to(in_last[None], (margin,)), doc_float], axis=0)
    total = jnp.zeros(product.shape, jnp.float32)
    for index in range(TAPS):
        same_doc = (padded_docs[index : index + row_count] == doc_float).astype(jnp.float32)
        total = (
            total
            + conv_taps[index].astype(jnp.float32)[None, :]
            * padded[index : index + row_count].astype(jnp.float32)
            * same_doc[:, None]
        )
    conv_out = (out_gate * total).astype(jnp.bfloat16)
    conv_columns, state_columns = (
        lax.all_gather(conv_out_weight, "sp", axis=1, tiled=True),
        lax.all_gather(state_out_weight, "sp", axis=1, tiled=True),
    )
    return lax.psum_scatter(
        (
            jnp.dot(conv_out, conv_columns, preferred_element_type=jnp.float32)
            + jnp.dot(ssm_out, state_columns, preferred_element_type=jnp.float32)
        ).astype(jnp.bfloat16),
        "tp",
        scatter_dimension=0,
        tiled=True,
    )


def solution(mesh):
    placed = (
        P(("fs", "sp"), "tp"),
        P(("fs", "sp")),
        P("tp"),
        P("sp", "tp"),
        P("sp", "tp"),
        P("sp", "tp"),
        P(None, "tp"),
        P("sp", "tp"),
        P("tp", None),
        P("tp", None),
        P("tp"),
        P("tp", None, None),
        P("tp", None, None),
        P("tp", None, None),
        P("tp", None, None),
        P("tp"),
        P("tp", "sp"),
        P("tp", "sp"),
    )
    return jax.shard_map(
        shards, mesh=mesh, in_specs=placed, out_specs=P(("fs", "sp", "tp"), None), check_vma=False
    )
```

```python
import functools
import math

import jax
import jax.numpy as jnp
from jax import lax
from jax.experimental import pallas as pl
from jax.experimental.pallas import tpu as pltpu
from jax.sharding import PartitionSpec as P

D = 2048
TAPS = 3
TILE = 8
REACHES = (1, 2, 4)


EPS = 1e-06


def from_behind(block, axis, distance):
    devices = range(lax.axis_size(axis))
    route = [(i - distance, i) for i in devices if i - distance in devices]
    return lax.ppermute(block, axis, route)


def ssm_constants(decay_rate, frequency, step_log, input_real, input_imag):
    step_size = jnp.exp(step_log)[:, None]
    damping = decay_rate * step_size
    turning = frequency * step_size
    fading = jnp.exp(-damping)
    coef_imag = fading * jnp.sin(turning)
    half_sine = jnp.sin(turning / 2.0)
    less_real = jnp.expm1(-damping) * jnp.cos(turning) - 2.0 * half_sine * half_sine
    denominator = decay_rate * decay_rate + frequency * frequency
    ratio_real = (-less_real * decay_rate + coef_imag * frequency) / denominator
    ratio_imag = (-coef_imag * decay_rate - less_real * frequency) / denominator
    bbar_real = ratio_real[..., None] * input_real - ratio_imag[..., None] * input_imag
    bbar_imag = ratio_real[..., None] * input_imag + ratio_imag[..., None] * input_real
    return (bbar_real, bbar_imag, damping.reshape(-1), turning.reshape(-1))


def spread(rows, group_size):
    lanes, state_size = rows.shape
    reps = lanes // group_size
    wide = jnp.concatenate([rows] * reps, axis=1)
    row = lax.broadcasted_iota(jnp.int32, wide.shape, 0) // group_size
    col = lax.broadcasted_iota(jnp.int32, wide.shape, 1) // state_size
    return jnp.where(row == col, wide, 0.0).astype(jnp.bfloat16)


def scan_rows(u, b_re, b_im, pow_re, pow_im, masks, start_re, start_im, keep):
    push_re = jnp.dot(u, b_re, preferred_element_type=jnp.float32)
    push_im = jnp.dot(u, b_im, preferred_element_type=jnp.float32)
    carry_re, carry_im = start_re, start_im
    for begin in range(0, u.shape[0], TILE):
        x_re = push_re[begin : begin + TILE]
        x_im = push_im[begin : begin + TILE]
        for slot, reach in enumerate(REACHES):
            m = masks[begin : begin + TILE, slot : slot + 1]
            p_re = pow_re[reach - 1 : reach] * m
            p_im = pow_im[reach - 1 : reach] * m
            s_re = pltpu.roll(x_re, reach, 0)
            s_im = pltpu.roll(x_im, reach, 0)
            x_re, x_im = x_re + (p_re * s_re - p_im * s_im), x_im + (p_re * s_im + p_im * s_re)
        m = masks[begin : begin + TILE, len(REACHES) : len(REACHES) + 1]
        p_re, p_im = pow_re * m, pow_im * m
        x_re, x_im = (
            x_re + (p_re * carry_re - p_im * carry_im),
            x_im + (p_re * carry_im + p_im * carry_re),
        )
        carry_re, carry_im = x_re[TILE - 1 :], x_im[TILE - 1 :]
        keep(begin, x_re, x_im)
    return carry_re, carry_im


def ends_body(group_size, u_ref, bre_ref, bim_ref, pre_ref, pim_ref, mask_ref, ere_ref, eim_ref):
    zero = jnp.zeros((1, pre_ref.shape[-1]), jnp.float32)
    end_re, end_im = scan_rows(
        u_ref[...],
        spread(bre_ref[...], group_size),
        spread(bim_ref[...], group_size),
        pre_ref[0],
        pim_ref[0],
        mask_ref[...],
        zero,
        zero,
        lambda begin, x_re, x_im: None,
    )
    ere_ref[0] = end_re
    eim_ref[0] = end_im


def join_body(keep_ref, take_ref, end_ref, dec_ref, sre_ref, sim_ref):
    dec_re, dec_im = dec_ref[0], dec_ref[1]
    s_re = jnp.zeros(dec_re.shape, jnp.float32)
    s_im = s_re
    for turn in range(end_ref.shape[0]):
        keep, take = keep_ref[turn], take_ref[turn]
        n_re = dec_re * s_re - dec_im * s_im + end_ref[turn, 0]
        n_im = dec_re * s_im + dec_im * s_re + end_ref[turn, 1]
        s_re, s_im = keep * s_re + take * n_re, keep * s_im + take * n_im
    sre_ref[...] = s_re
    sim_ref[...] = s_im


def mix_body(
    group_size, u_ref, bre_ref, bim_ref, cre_ref, cim_ref, pre_ref, pim_ref, mask_ref,
    sre_ref, sim_ref, skip_ref, out_ref, hre_ref, him_ref,
):
    def keep(begin, x_re, x_im):
        hre_ref[begin : begin + TILE, :] = x_re
        him_ref[begin : begin + TILE, :] = x_im

    u = u_ref[...]
    scan_rows(
        u,
        spread(bre_ref[...], group_size),
        spread(bim_ref[...], group_size),
        pre_ref[0],
        pim_ref[0],
        mask_ref[...],
        sre_ref[0],
        sim_ref[0],
        keep,
    )
    along = (((1,), (1,)), ((), ()))
    y = lax.dot_general(
        hre_ref[...].astype(jnp.bfloat16),
        spread(cre_ref[...], group_size),
        along,
        preferred_element_type=jnp.float32,
    ) - lax.dot_general(
        him_ref[...].astype(jnp.bfloat16),
        spread(cim_ref[...], group_size),
        along,
        preferred_element_type=jnp.float32,
    )
    y = y + skip_ref[...] * u.astype(jnp.float32)
    out_ref[...] = jax.nn.gelu(y, approximate=True).astype(jnp.bfloat16)


def block_specs(rows, lanes, state_size, span):
    return dict(
        u=pl.BlockSpec((rows, lanes), lambda j: (0, j)),
        mat=pl.BlockSpec((lanes, state_size), lambda j: (j, 0)),
        pow=pl.BlockSpec((1, TILE, span), lambda j: (j, 0, 0)),
        mask=pl.BlockSpec((rows, len(REACHES) + 1), lambda j: (0, 0)),
        state=pl.BlockSpec((1, 1, span), lambda j: (j, 0, 0)),
        skip=pl.BlockSpec((1, lanes), lambda j: (0, j)),
    )


def shards(
    tokens,
    documents,
    norm_gain,
    out_gate_weight,
    in_gate_weight,
    value_weight,
    conv_taps,
    state_in_weight,
    decay_rate,
    frequency,
    step_log,
    input_real,
    input_imag,
    readout_real,
    readout_imag,
    skip_gain,
    conv_out_weight,
    state_out_weight,
):
    row_count = tokens.shape[0]
    groups, state_size = decay_rate.shape
    group_size = input_real.shape[2]
    values = tokens.astype(jnp.float32)
    totals = lax.psum(jnp.sum(values * values, axis=1), "tp")
    scaled = values * lax.rsqrt(totals / D + EPS)[:, None] * norm_gain.astype(jnp.float32)[None, :]
    normed = lax.all_gather(scaled.astype(jnp.bfloat16), "tp", axis=1, tiled=True)
    bbar_real, bbar_imag, damping, turning = ssm_constants(
        decay_rate, frequency, step_log, input_real, input_imag
    )
    doc_float = documents.astype(jnp.float32)
    devices = lax.axis_size("sp")
    near = math.gcd(devices, 4)
    rows_of = [[i * near + j for j in range(near)] for i in range(devices // near)]
    columns_of = [[i * near + j for i in range(devices // near)] for j in range(near)]
    weights = (out_gate_weight, in_gate_weight, value_weight, state_in_weight)
    strip = out_gate_weight.shape[1] // near
    strips = jnp.stack(
        [
            jnp.concatenate([w[:, j * strip : (j + 1) * strip] for w in weights], axis=1)
            for j in range(near)
        ]
    )
    strips = lax.all_to_all(strips, "sp", 0, 0, axis_index_groups=rows_of, tiled=True)
    strips = lax.all_gather(
        strips.reshape(-1, len(weights) * strip),
        "sp",
        axis=0,
        axis_index_groups=columns_of,
        tiled=True,
    )
    near_rows = lax.all_gather(normed, "sp", axis=0, axis_index_groups=rows_of, tiled=True)
    sums = jnp.dot(near_rows, strips, preferred_element_type=jnp.float32).astype(jnp.bfloat16)
    sums = lax.all_to_all(
        sums.reshape(near, row_count, -1), "sp", 0, 0, axis_index_groups=rows_of, tiled=True
    )
    gate_sum, inner_sum, value_sum, driven = (
        jnp.concatenate([sums[j, :, k * strip : (k + 1) * strip] for j in range(near)], axis=1)
        for k in range(len(weights))
    )
    place = lax.axis_index("sp")
    in_last = jnp.where(place > 0, from_behind(doc_float[-1:], "sp", 1)[0], -1.0)
    lanes = math.gcd(groups * group_size, 128)
    blocks = groups * group_size // lanes
    span = lanes // group_size * state_size
    order = jnp.arange(row_count)
    columns = [
        (order % TILE >= reach) & (documents == jnp.roll(documents, reach)) for reach in REACHES
    ]
    before = jnp.concatenate([in_last[None], doc_float[TILE - 1 : -1 : TILE]])
    columns.append(doc_float == jnp.repeat(before, TILE))
    masks = jnp.stack(columns, axis=1).astype(jnp.float32)
    counts = jnp.arange(1, TILE + 1, dtype=jnp.float32)[None, :, None]
    damp = damping.reshape(blocks, 1, span)
    turn = turning.reshape(blocks, 1, span)
    fade = jnp.exp(-counts * damp)
    pow_re, pow_im = fade * jnp.cos(counts * turn), fade * jnp.sin(counts * turn)
    damp, turn = damp[:, 0], turn[:, 0]
    whole = jnp.exp(-row_count * damp)
    decay = jnp.stack([whole * jnp.cos(row_count * turn), whole * jnp.sin(row_count * turn)])
    b_re = jnp.swapaxes(bbar_real, 1, 2).reshape(groups * group_size, state_size)
    b_im = jnp.swapaxes(bbar_imag, 1, 2).reshape(groups * group_size, state_size)
    c_re = readout_real.reshape(groups * group_size, state_size)
    c_im = readout_imag.reshape(groups * group_size, state_size)
    spec = block_specs(row_count, lanes, state_size, span)
    state_shape = jax.ShapeDtypeStruct((blocks, 1, span), jnp.float32)
    ends = pl.pallas_call(
        functools.partial(ends_body, group_size),
        grid=(blocks,),
        in_specs=[spec[k] for k in ("u", "mat", "mat", "pow", "pow", "mask")],
        out_specs=[spec["state"]] * 2,
        out_shape=[state_shape] * 2,
        name="ends",
    )(driven, b_re, b_im, pow_re, pow_im, masks)
    packed = jnp.concatenate(
        [e.reshape(blocks, span) for e in ends] + [jnp.broadcast_to(doc_float[-1], (1, span))]
    )
    packed = lax.all_gather(packed, "sp", axis_index_groups=rows_of)
    packed = lax.all_gather(packed, "sp", axis_index_groups=columns_of)
    packed = packed.reshape(devices, 2 * blocks + 1, span)
    ends = packed[:, : 2 * blocks].reshape(devices, 2, blocks, span)
    lasts = packed[:, 2 * blocks, 0]
    source = jnp.arange(devices)
    take = ((source < place) & (lasts == in_last)).astype(jnp.float32)
    later = (source >= place).astype(jnp.float32)
    scalar = pl.BlockSpec(memory_space=pltpu.SMEM)
    vector = pl.BlockSpec(memory_space=pltpu.VMEM)
    start_re, start_im = pl.pallas_call(
        join_body,
        in_specs=[scalar, scalar, vector, vector],
        out_specs=[vector] * 2,
        out_shape=[jax.ShapeDtypeStruct((blocks, span), jnp.float32)] * 2,
        name="join",
    )(later, take, ends, decay)
    ssm_out = pl.pallas_call(
        functools.partial(mix_body, group_size),
        grid=(blocks,),
        in_specs=[
            spec[k]
            for k in (
                "u", "mat", "mat", "mat", "mat", "pow", "pow", "mask", "state", "state", "skip",
            )
        ],
        out_specs=spec["u"],
        out_shape=jax.ShapeDtypeStruct(driven.shape, jnp.bfloat16),
        scratch_shapes=[pltpu.VMEM((row_count, span), jnp.float32)] * 2,
        name="mix",
    )(
        driven, b_re, b_im, c_re, c_im, pow_re, pow_im, masks,
        start_re[:, None], start_im[:, None], skip_gain[None],
    )
    out_gate = gate_sum.astype(jnp.bfloat16).astype(jnp.float32)
    in_gate = inner_sum.astype(jnp.bfloat16).astype(jnp.float32)
    value = value_sum.astype(jnp.bfloat16).astype(jnp.float32)
    product = (in_gate * value).astype(jnp.bfloat16)
    margin = TAPS - 1
    tail_same = documents[row_count - margin :] == documents[-1]
    tail_rows = jnp.where(
        tail_same[:, None], product[row_count - margin :], jnp.zeros_like(product[:margin])
    )
    rim_rows = from_behind(tail_rows, "sp", 1)
    padded = jnp.concatenate([rim_rows, product], axis=0)
    padded_docs = jnp.concatenate([jnp.broadcast_to(in_last[None], (margin,)), doc_float], axis=0)
    total = jnp.zeros(product.shape, jnp.float32)
    for index in range(TAPS):
        same_doc = (padded_docs[index : index + row_count] == doc_float).astype(jnp.float32)
        total = (
            total
            + conv_taps[index].astype(jnp.float32)[None, :]
            * padded[index : index + row_count].astype(jnp.float32)
            * same_doc[:, None]
        )
    conv_out = (out_gate * total).astype(jnp.bfloat16)
    columns = jnp.concatenate([conv_out_weight, state_out_weight], axis=0).T
    columns = lax.all_gather(columns, "sp", axis=0, axis_index_groups=columns_of, tiled=True)
    mixers = jnp.concatenate([conv_out, ssm_out], axis=1)
    mixers = lax.all_gather(mixers, "sp", axis=0, axis_index_groups=rows_of, tiled=True)
    part = lax.dot_general(
        mixers, columns, (((1,), (1,)), ((), ())), preferred_element_type=jnp.float32
    ).astype(jnp.bfloat16)
    part = lax.all_to_all(
        part.reshape(near, row_count, -1), "sp", 0, 0, axis_index_groups=rows_of, tiled=True
    )
    part = part.reshape(near, row_count, devices // near, -1)
    part = part.transpose(1, 2, 0, 3).reshape(row_count, -1)
    return lax.psum_scatter(part, "tp", scatter_dimension=0, tiled=True)


def solution(mesh):
    placed = (
        P(("fs", "sp"), "tp"),
        P(("fs", "sp")),
        P("tp"),
        P("sp", "tp"),
        P("sp", "tp"),
        P("sp", "tp"),
        P(None, "tp"),
        P("sp", "tp"),
        P("tp", None),
        P("tp", None),
        P("tp"),
        P("tp", None, None),
        P("tp", None, None),
        P("tp", None, None),
        P("tp", None, None),
        P("tp"),
        P("tp", "sp"),
        P("tp", "sp"),
    )
    return jax.shard_map(
        shards, mesh=mesh, in_specs=placed, out_specs=P(("fs", "sp", "tp"), None), check_vma=False
    )
```
